32 devices in a mesh: kv: 8 (over z, x), tp: 4 (over y, core).
Axes of the slice: x: 2, y: 2, z: 4, core: 2. Of those that a mesh axis runs over, the one named last changes fastest.
Arguments:
- queries: bfloat16 [64, 4, 8, 128], P('kv', None, 'tp'), may hold values from -6 to 6
- keys: bfloat16 [64, 4, 8, 128], P('kv', None, 'tp'), may hold values from -6 to 6
- values: bfloat16 [64, 4, 8, 256], P('kv', None, 'tp'), may hold values from -6 to 6
- in_gate: float32 [64, 4, 8], P('kv', None, 'tp'), may hold values from -6 to 6
- forget_pre: float32 [64, 4, 8], P('kv', None, 'tp'), may hold values from -1 to 5
- old_keys: bfloat16 [64, 4, 8, 128], P('kv', None, 'tp'), may hold values from -6 to 6
- old_values: bfloat16 [64, 4, 8, 256], P('kv', None, 'tp'), may hold values from -6 to 6
- old_in_gate: float32 [64, 4, 8], P('kv', None, 'tp'), may hold values from -6 to 6
- old_forget: float32 [64, 4, 8], P('kv', None, 'tp'), may hold values from -1 to 5
- accepted: int32 [64], P('kv'), may hold values from 0 to 4
- state_mem: float32 [64, 8, 128, 256], P('kv', 'tp'), may hold values from -4 to 4
- state_norm: float32 [64, 8, 128], P('kv', 'tp'), may hold values from -6 to 6
- state_max: float32 [64, 8], P('kv', 'tp'), may hold values from -4 to 4
- norm_gain: float32 [8, 256], P('tp'), may hold values from 0.1 to 1.9
- out_weight: bfloat16 [2048, 2048], P('tp', 'kv'), may hold values from -0.125 to 0.125
Outputs:
- mixed: bfloat16 [64, 4, 2048], P('kv', 'tp')
- new_mem: float32 [64, 8, 128, 256], P('kv', 'tp')
- new_norm: float32 [64, 8, 128], P('kv', 'tp')
- new_max: float32 [64, 8], P('kv', 'tp')
The draws below stay inside these ranges and needn't reach their ends.
Inputs may be any that keep to these rules, and one draw needn't show every extreme that they name: How many of the last step's 4 proposals of a sequence were accepted.
All inputs are finite; a program needn't handle non-finite values.
Results may differ from the reference program's by a relative error of at most 0.0068.
Values may be sent and summed in bfloat16 or wider, within the bound.
A program may use at most 64 MiB of HBM per device.

```python
import jax
import jax.numpy as jnp
from jax import lax

D = 2048
HEADS = 8
DK = 128
DV = 256
PROPOSALS = 4
SEQS = 64
HV = 2048


def with_ends(array, stream_key, least, largest):
    place = [jax.random.randint(jax.random.fold_in(stream_key, axis), (), 0, length) for axis, length in enumerate(array.shape)]
    main_axis = array.shape.index(max(array.shape))
    neighbour = place[:main_axis] + [(place[main_axis] + 1) % array.shape[main_axis]] + place[main_axis + 1:]
    return array.at[tuple(place)].set(least).at[tuple(neighbour)].set(largest)


def levels(own_key, dims, shards, smallest, high):
    gain, own = 1.0, jax.random.fold_in(own_key, 6)
    for axis_at, shards_of in shards:
        steps = jnp.exp(jax.random.uniform(jax.random.fold_in(own, axis_at), (shards_of,), jnp.float32, smallest / len(shards), high / len(shards)))
        gain = gain * jnp.repeat(steps, dims[axis_at] // shards_of).reshape([-1 if axis == axis_at else 1 for axis in range(len(dims))])
    return gain


def normal_values(rng, dims, deviation, reach, pieces=(), kind=jnp.bfloat16):
    gain = levels(rng, dims, pieces, -0.22, 0.18) if pieces else 1.0
    values = jax.random.normal(rng, dims, jnp.float32) * deviation * gain
    return jnp.minimum(jnp.maximum(values, -reach), reach).astype(kind)


def setup_inputs(seed: int = 0) -> dict:
    streams_of = jax.random.split(jax.random.key(seed), 16)
    queries = normal_values(streams_of[0], (SEQS, PROPOSALS, HEADS, DK), 1.0, 6.0, ((0, 8), (2, 4)))
    keys = normal_values(streams_of[1], (SEQS, PROPOSALS, HEADS, DK), 1.0, 6.0, ((0, 8), (2, 4)))
    values = normal_values(streams_of[2], (SEQS, PROPOSALS, HEADS, DV), 1.0, 6.0, ((0, 8), (2, 4)))
    in_gate = normal_values(streams_of[3], (SEQS, PROPOSALS, HEADS), 1.0, 6.0, ((0, 8), (2, 4)), jnp.float32)
    forget_pre = jnp.clip(-1.0 + 6.0 * jax.random.uniform(streams_of[4], (SEQS, PROPOSALS, HEADS), jnp.float32) ** levels(streams_of[4], (SEQS, PROPOSALS, HEADS), ((0, 8), (2, 4)), -0.2, 0.2), -1.0, 5.0)
    old_keys = normal_values(streams_of[5], (SEQS, PROPOSALS, HEADS, DK), 1.0, 6.0, ((0, 8), (2, 4)))
    old_values = normal_values(streams_of[6], (SEQS, PROPOSALS, HEADS, DV), 1.0, 6.0, ((0, 8), (2, 4)))
    old_in_gate = normal_values(streams_of[7], (SEQS, PROPOSALS, HEADS), 1.0, 6.0, ((0, 8), (2, 4)), jnp.float32)
    old_forget = jnp.clip(-1.0 + 6.0 * jax.random.uniform(streams_of[8], (SEQS, PROPOSALS, HEADS), jnp.float32) ** levels(streams_of[8], (SEQS, PROPOSALS, HEADS), ((0, 8), (2, 4)), -0.2, 0.2), -1.0, 5.0)
    accepted = with_ends(jax.random.randint(streams_of[9], (SEQS,), 0, PROPOSALS + 1), jax.random.fold_in(streams_of[9], 1), 0, PROPOSALS).astype(jnp.int32)
    state_mem = normal_values(streams_of[10], (SEQS, HEADS, DK, DV), 0.3, 4.0, ((0, 8), (1, 4)), jnp.float32)
    state_norm = normal_values(streams_of[11], (SEQS, HEADS, DK), 0.5, 6.0, ((0, 8), (1, 4)), jnp.float32)
    state_max = normal_values(streams_of[12], (SEQS, HEADS), 1.0, 4.0, ((0, 8), (1, 4)), jnp.float32)
    norm_gain = jnp.clip(1.0 + 0.18 * jax.random.normal(streams_of[13], (HEADS, DV), jnp.float32), 0.1, 1.9)
    out_weight = normal_values(streams_of[14], (HV, D), HV ** -0.5, 0.125, ((0, 4), (1, 8)))
    return dict(queries=queries, keys=keys, values=values, in_gate=in_gate, forget_pre=forget_pre, old_keys=old_keys, old_values=old_values, old_in_gate=old_in_gate, old_forget=old_forget, accepted=accepted, state_mem=state_mem, state_norm=state_norm, state_max=state_max, norm_gain=norm_gain, out_weight=out_weight)


HIGH = lax.Precision.HIGHEST

def cell(queries, keys, values, in_gates, log_forget, memory, normal, stab):
    length = in_gates.shape[-1]
    causal = jnp.tril(jnp.ones((length, length), dtype=bool))
    cumul = jnp.cumsum(log_forget, axis=-1)
    logd = jnp.where(causal, cumul[:, :, None] - cumul[:, None, :] + in_gates[:, None, :], -jnp.inf)
    inter = cumul + stab[:, None]
    m_row = jnp.maximum(inter, lax.optimization_barrier(jnp.max(logd, axis=-1)))
    scores = jnp.einsum('hld,hsd->hls', queries, keys, precision=HIGH) * jnp.exp(logd - m_row[..., None])
    w_inter = jnp.exp(inter - m_row)
    num = w_inter[..., None] * jnp.einsum('hld,hde->hle', queries, memory, precision=HIGH) + jnp.einsum('hls,hse->hle', scores, values, precision=HIGH)
    den = w_inter * jnp.einsum('hld,hd->hl', queries, normal, precision=HIGH) + lax.optimization_barrier(jnp.sum(scores, axis=-1))
    hidden = num / jnp.maximum(jnp.abs(den), 1.0)[..., None]
    m_new = m_row[:, -1]
    g_state = jnp.exp(cumul[:, -1] + stab - m_new)
    g_tok = jnp.exp(cumul[:, -1:] - cumul + in_gates - m_new[:, None])
    mem_new = g_state[:, None, None] * memory + jnp.einsum('hld,hle->hde', g_tok[..., None] * keys, values, precision=HIGH)
    norm_new = g_state[:, None] * normal + jnp.einsum('hl,hld->hd', g_tok, keys, precision=HIGH)
    return (hidden, mem_new, norm_new, m_new)

def one_sequence(items):
    queries, keys, values, in_gate, forget_pre, old_keys, old_values, old_in_gate, old_forget, accepted, memory, normal, stab, norm_gain = items
    props = queries.shape[0]
    live = jnp.arange(props, dtype=jnp.int32) < accepted
    gates = jnp.concatenate([jnp.where(live[:, None], old_in_gate, -jnp.inf), in_gate], axis=0)
    forget = jnp.concatenate([jnp.where(live[:, None], jax.nn.log_sigmoid(old_forget), 0.0), jax.nn.log_sigmoid(forget_pre)], axis=0)
    scale = queries.shape[-1] ** (-0.5)
    qrun = jnp.concatenate([jnp.zeros(queries.shape, jnp.float32), queries.astype(jnp.float32) * scale], axis=0)
    krun = jnp.concatenate([old_keys, keys], axis=0).astype(jnp.float32)
    vrun = jnp.concatenate([old_values, values], axis=0).astype(jnp.float32)
    hidden, mem_new, norm_new, m_new = cell(jnp.swapaxes(qrun, 0, 1), jnp.swapaxes(krun, 0, 1), jnp.swapaxes(vrun, 0, 1), gates.T, forget.T, memory, normal, stab)
    hidden = hidden[:, props:, :]
    mean = lax.optimization_barrier(jnp.mean(hidden, -1, keepdims=True))
    var = lax.optimization_barrier(jnp.mean(jnp.square(hidden - mean), -1, keepdims=True))
    normed = (hidden - mean) * lax.rsqrt(var + 1e-05) * norm_gain[:, None, :]
    flat = jnp.swapaxes(normed, 0, 1).reshape(props, -1).astype(jnp.bfloat16)
    return (flat, mem_new, norm_new, m_new)

def reference(queries, keys, values, in_gate, forget_pre, old_keys, old_values, old_in_gate, old_forget, accepted, state_mem, state_norm, state_max, norm_gain, out_weight):

    def apply(items):
        return one_sequence(items + (norm_gain,))
    hidden, new_mem, new_norm, new_max = lax.map(apply, (queries, keys, values, in_gate, forget_pre, old_keys, old_values, old_in_gate, old_forget, accepted, state_mem, state_norm, state_max))
    seqs, props, width = hidden.shape
    flat = hidden.reshape(seqs * props, width)
    total = jnp.dot(flat, out_weight, preferred_element_type=jnp.float32)
    mixed = total.astype(jnp.bfloat16).reshape(seqs, props, -1)
    return (mixed, new_mem, new_norm, new_max)
```

```python
import functools

import jax
import jax.numpy as jnp
from jax import lax
from jax.experimental import pallas as pl
from jax.experimental.pallas import tpu as pltpu
from jax.sharding import PartitionSpec as P

MESH = pl.DeviceIdType.MESH
F32 = jnp.float32
BF16 = jnp.bfloat16
PAIR = 2


def log_sigmoid(x):
    return jnp.minimum(x, 0.0) - jnp.log1p(jnp.exp(-jnp.abs(x)))


def split(x):
    hi = x.astype(BF16)
    return hi, (x - hi.astype(F32)).astype(BF16)


def dot(a, b):
    return jnp.dot(a, b, preferred_element_type=F32)


def kernel(
    zs, tps,
    q_ref, k_ref, v_ref, ig_ref, fg_ref, ok_ref, ov_ref, oig_ref, ofg_ref, acc_ref,
    norm_ref, max_ref, gain_ref, mem_hbm, w_hbm,
    mixed_ref, newmem_ref, newnorm_ref, newmax_ref,
    mem, w_own, w_peer, kf, vf, qf, rows, y, ck, hid, part, got,
    mem_sem, w_sem, wx_sems, hid_send, hid_recv, part_send, part_recv,
):
    seqs, heads, dk, dv = newmem_ref.shape
    props = ig_ref.shape[0]
    run = 2 * props
    stride = props * heads
    wide = dv // 128
    kv, tp = lax.axis_index("kv"), lax.axis_index("tp")
    z, x = kv // PAIR, kv % PAIR

    def device(z_at, t_at):
        return {"kv": z_at * PAIR + x, "tp": t_at}

    others = [(dz, dt) for dz in range(zs) for dt in range(tps) if dz or dt]

    def at(dz, dt):
        return lax.rem(z + dz, zs), lax.rem(tp + dt, tps)

    mem_in = [
        pltpu.make_async_copy(mem_hbm.at[s], mem.at[s], mem_sem.at[s]) for s in range(seqs)
    ]
    for copy in mem_in:
        copy.start()
    w_in = pltpu.make_async_copy(w_hbm, w_own, w_sem)
    w_in.start()

    peer = {"kv": z * PAIR + (1 - x), "tp": tp}
    barrier = pltpu.get_barrier_semaphore()
    pl.semaphore_signal(barrier, inc=1, device_id=peer, device_id_type=MESH)
    for dz, dt in others:
        pl.semaphore_signal(barrier, inc=1, device_id=device(*at(dz, dt)), device_id_type=MESH)

    accepted = acc_ref[...]
    state_max = max_ref[...]
    ig, b, total = [], [], None
    for t in range(run):
        if t < props:
            live = t < accepted
            ig.append(jnp.where(live, oig_ref[t], -jnp.inf))
            lf = jnp.where(live, log_sigmoid(ofg_ref[t]), 0.0)
        else:
            ig.append(ig_ref[t - props])
            lf = log_sigmoid(fg_ref[t - props])
        total = lf if total is None else total + lf
        b.append(total)
    index = {}
    count = 0
    for t in range(props, run):
        logd = [b[t] - b[s] + ig[s] for s in range(t + 1)]
        inter = b[t] + state_max
        m_row = functools.reduce(jnp.maximum, logd, inter)
        for s in list(range(t + 1)) + ["w"]:
            row = jnp.exp((inter if s == "w" else logd[s]) - m_row)
            rows[count * heads : (count + 1) * heads, 0:seqs] = row
            index[t, s] = count * heads
            count += 1
    newmax_ref[...] = m_row
    columns = rows[...].T[0:seqs]

    def column(t, s, h):
        return columns[:, index[t, s] + h : index[t, s] + h + 1]

    qf[...] = q_ref[...].astype(F32)
    kf[0] = ok_ref[...].astype(F32)
    kf[1] = k_ref[...].astype(F32)
    for s in range(seqs):
        for p in range(props):
            r = s * stride + p * heads
            for c in range(wide):
                lanes = slice(c * 128, (c + 1) * 128)
                vf[0, c, r : r + heads, :] = ov_ref[s, p, :, lanes].astype(F32)
                vf[1, c, r : r + heads, :] = v_ref[s, p, :, lanes].astype(F32)

    def pick(ref, p, h):
        return ref[pl.ds(p * heads + h, seqs, stride=stride), :]

    def pick_wide(ref, p, h):
        return jnp.concatenate([pick(ref.at[c], p, h) for c in range(wide)], axis=-1)

    def run_pick(ref, t, h):
        return pick(ref.at[t // props], t % props, h)

    scale = dk ** (-0.5)
    scores, dens, norms = {}, {}, {}
    for h in range(heads):
        ks = [run_pick(kf, s, h) for s in range(run)]
        normal = norm_ref[pl.ds(h, seqs, stride=heads), :]
        for t in range(props, run):
            q = pick(qf, t - props, h) * scale
            den = column(t, "w", h) * jnp.sum(q * normal, axis=-1, keepdims=True)
            for s in range(t + 1):
                score = jnp.sum(q * ks[s], axis=-1, keepdims=True) * column(t, s, h)
                scores[t, s, h] = score
                den = den + score
            dens[t, h] = jnp.maximum(jnp.abs(den), 1.0)
        norm = column(run - 1, "w", h) * normal
        for s in range(run):
            c = column(run - 1, s, h) * ks[s]
            ck.at[s // props][pl.ds((s % props) * heads + h, seqs, stride=stride), :] = c
            norm = norm + c
        newnorm_ref[pl.ds(h, seqs, stride=heads), :] = norm

    pl.semaphore_wait(barrier, len(others) + 1)
    w_swap = pltpu.make_async_remote_copy(
        src_ref=w_hbm, dst_ref=w_peer, send_sem=wx_sems.at[0], recv_sem=wx_sems.at[1],
        device_id=peer, device_id_type=MESH,
    )
    w_swap.start()

    parity = lax.broadcasted_iota(jnp.int32, (stride, 1), 0) % heads
    for s in range(seqs):
        mem_in[s].wait()
        q = q_ref[s * stride : (s + 1) * stride, :]
        out = None
        for h in range(heads):
            hi, lo = split(mem[s, h])
            term = dot(q, hi) + dot(q, lo)
            out = term if h == 0 else jnp.where(parity == h, term, out)
        for c in range(wide):
            y[c, s * stride : (s + 1) * stride, :] = out[:, c * 128 : (c + 1) * 128]

    for h in range(heads):
        vs = [pick_wide(vf.at[s // props], s % props, h) for s in range(run)]
        gain = gain_ref[h : h + 1, :]
        normed = []
        for t in range(props, run):
            num = (column(t, "w", h) * scale) * pick_wide(y, t - props, h)
            for s in range(t + 1):
                num = num + scores[t, s, h] * vs[s]
            cell = num / dens[t, h]
            mean = jnp.mean(cell, axis=-1, keepdims=True)
            cell = cell - mean
            var = jnp.mean(jnp.square(cell), axis=-1, keepdims=True)
            normed.append(cell * lax.rsqrt(var + 1e-05) * gain)
        hid[z, :, h * dv : (h + 1) * dv] = jnp.concatenate(normed, axis=0).astype(BF16)

    def hid_copy(slot, to):
        return pltpu.make_async_remote_copy(
            src_ref=hid.at[slot], dst_ref=hid.at[slot], send_sem=hid_send.at[to],
            recv_sem=hid_recv.at[slot], device_id=device(to, tp), device_id_type=MESH,
        )

    order = sorted(range(1, zs), key=lambda d: -min(d, zs - d))
    for d in order:
        hid_copy(z, lax.rem(z + d, zs)).start()

    def part_copy(slot, half, t_at, src_half):
        return pltpu.make_async_remote_copy(
            src_ref=part.at[slot, half, t_at], dst_ref=got.at[tp, z, half],
            send_sem=part_send.at[slot, half, t_at], recv_sem=part_recv.at[tp, z, half],
            device_id=device(slot, t_at), device_id_type=MESH,
        )

    def project(slot, half, weights, own):
        terms = dot(hid[slot], weights[...])
        for p in range(props):
            part[slot, half, p] = terms[p * seqs : (p + 1) * seqs].astype(BF16)
        for dt in range(tps):
            if not (own and dt == 0):
                part_copy(slot, half, lax.rem(tp + dt, tps), half).start()
        if own:
            got[tp, z, half] = part[slot, half, tp]

    w_in.wait()
    project(z, x, w_own, True)

    for s in range(seqs):
        at_s = pl.ds(s * stride, stride)
        values = jnp.concatenate(
            [
                jnp.concatenate([vf[old, c, at_s, :] for c in range(wide)], axis=-1)
                for old in (0, 1, 0, 1)
            ],
            axis=0,
        ).astype(BF16)
        keys = jnp.concatenate([ck[0, at_s, :], ck[1, at_s, :]], axis=0)
        both = lax.broadcasted_iota(jnp.int32, (2 * stride, 1), 0) % heads
        for h in range(heads):
            hi, lo = split(jnp.where(both == h, keys, 0.0))
            update = lax.dot_general(
                jnp.concatenate([hi, lo], axis=0), values, (((0,), (0,)), ((), ())),
                preferred_element_type=F32,
            )
            newmem_ref[s, h] = column(run - 1, "w", h)[s : s + 1] * mem[s, h] + update

    for d in range(1, zs):
        slot = lax.rem(z + d, zs)
        hid_copy(slot, slot).wait_recv()
        project(slot, x, w_own, False)
    w_swap.wait_recv()
    for d in range(zs):
        project(lax.rem(z + d, zs), 1 - x, w_peer, d == 0)

    for dz, dt in others:
        z_at, t_at = at(dz, dt)
        for half in range(PAIR):
            pltpu.make_async_remote_copy(
                src_ref=part.at[z_at, half, t_at], dst_ref=got.at[t_at, z_at, half],
                send_sem=part_send.at[z_at, half, t_at], recv_sem=part_recv.at[t_at, z_at, half],
                device_id=device(z_at, t_at), device_id_type=MESH,
            ).wait_recv()
    width = got.shape[-1]
    for z_at in range(zs):
        for half in range(PAIR):
            out = got[0, z_at, half].astype(F32)
            for t in range(1, tps):
                out = out + got[t, z_at, half].astype(F32)
            at_c = (z_at * PAIR + half) * width
            mixed_ref[:, at_c : at_c + width] = out.astype(BF16)

    w_swap.wait_send()
    for d in range(1, zs):
        hid_copy(z, lax.rem(z + d, zs)).wait_send()
    for dz, dt in others:
        z_at, t_at = at(dz, dt)
        for half in range(PAIR):
            part_copy(z_at, half, t_at, half).wait_send()


def on_device(
    kvs, tps,
    queries, keys, values, in_gate, forget_pre, old_keys, old_values, old_in_gate, old_forget,
    accepted, state_mem, state_norm, state_max, norm_gain, out_weight,
):
    seqs, props, heads, dk = queries.shape
    dv = values.shape[-1]
    rows, cols = out_weight.shape
    zs = kvs // PAIR
    flat = (seqs * props * heads, dk)
    gates = [jnp.transpose(g, (1, 2, 0)) for g in (in_gate, forget_pre, old_in_gate, old_forget)]
    vmem = pl.BlockSpec(memory_space=pltpu.VMEM)
    hbm = pl.BlockSpec(memory_space=pl.ANY)
    sem = pltpu.SemaphoreType.DMA
    mixed, new_mem, new_norm, new_max = pl.pallas_call(
        functools.partial(kernel, zs, tps),
        out_shape=(
            jax.ShapeDtypeStruct((seqs, kvs * cols), BF16),
            jax.ShapeDtypeStruct(state_mem.shape, F32),
            jax.ShapeDtypeStruct((seqs * heads, dk), F32),
            jax.ShapeDtypeStruct((heads, seqs), F32),
        ),
        in_specs=[vmem] * 13 + [hbm] * 2,
        out_specs=(vmem,) * 4,
        scratch_shapes=[
            pltpu.VMEM(state_mem.shape, F32),
            pltpu.VMEM((rows, cols), BF16),
            pltpu.VMEM((rows, cols), BF16),
            pltpu.VMEM((2,) + flat, F32),
            pltpu.VMEM((2, dv // 128, flat[0], 128), F32),
            pltpu.VMEM(flat, F32),
            pltpu.VMEM((128, 128), F32),
            pltpu.VMEM((dv // 128, flat[0], 128), F32),
            pltpu.VMEM((2,) + flat, F32),
            pltpu.VMEM((zs, props * seqs, heads * dv), BF16),
            pltpu.VMEM((zs, PAIR, props, seqs, cols), BF16),
            pltpu.VMEM((tps, zs, PAIR, seqs, cols), BF16),
            sem((seqs,)),
            sem,
            sem((2,)),
            sem((zs,)),
            sem((zs,)),
            sem((zs, PAIR, props)),
            sem((tps, zs, PAIR)),
        ],
        compiler_params=pltpu.CompilerParams(collective_id=0, has_side_effects=True),
    )(
        queries.reshape(flat), keys.reshape(flat), values, gates[0], gates[1],
        old_keys.reshape(flat), old_values, gates[2], gates[3], accepted.reshape(1, seqs),
        state_norm.reshape(seqs * heads, dk), state_max.T, norm_gain, state_mem, out_weight,
    )
    return (
        mixed.reshape(seqs, 1, kvs * cols),
        new_mem,
        new_norm.reshape(state_norm.shape),
        new_max.T,
    )


HIGH = lax.Precision.HIGHEST


def cell(queries, keys, values, in_gates, log_forget, memory, normal, stab):
    length = in_gates.shape[-1]
    causal = jnp.tril(jnp.ones((length, length), dtype=bool))
    cumul = jnp.cumsum(log_forget, axis=-1)
    logd = jnp.where(causal, cumul[:, :, None] - cumul[:, None, :] + in_gates[:, None, :], -jnp.inf)
    inter = cumul + stab[:, None]
    m_row = jnp.maximum(inter, jnp.max(logd, axis=-1))
    scores = jnp.einsum("hld,hsd->hls", queries, keys, precision=HIGH) * jnp.exp(
        logd - m_row[..., None]
    )
    w_inter = jnp.exp(inter - m_row)
    num = w_inter[..., None] * jnp.einsum(
        "hld,hde->hle", queries, memory, precision=HIGH
    ) + jnp.einsum("hls,hse->hle", scores, values, precision=HIGH)
    den = w_inter * jnp.einsum("hld,hd->hl", queries, normal, precision=HIGH) + jnp.sum(
        scores, axis=-1
    )
    hidden = num / jnp.maximum(jnp.abs(den), 1.0)[..., None]
    m_new = m_row[:, -1]
    g_state = jnp.exp(cumul[:, -1] + stab - m_new)
    g_tok = jnp.exp(cumul[:, -1:] - cumul + in_gates - m_new[:, None])
    mem_new = g_state[:, None, None] * memory + jnp.einsum(
        "hld,hle->hde", g_tok[..., None] * keys, values, precision=HIGH
    )
    norm_new = g_state[:, None] * normal + jnp.einsum("hl,hld->hd", g_tok, keys, precision=HIGH)
    return (hidden, mem_new, norm_new, m_new)


def one_sequence(
    queries,
    keys,
    values,
    in_gate,
    forget_pre,
    old_keys,
    old_values,
    old_in_gate,
    old_forget,
    accepted,
    memory,
    normal,
    stab,
    norm_gain,
):
    props = queries.shape[0]
    live = jnp.arange(props, dtype=jnp.int32) < accepted
    gates = jnp.concatenate([jnp.where(live[:, None], old_in_gate, -jnp.inf), in_gate], axis=0)
    forget = jnp.concatenate(
        [
            jnp.where(live[:, None], jax.nn.log_sigmoid(old_forget), 0.0),
            jax.nn.log_sigmoid(forget_pre),
        ],
        axis=0,
    )
    scale = queries.shape[-1] ** (-0.5)
    qrun = jnp.concatenate(
        [jnp.zeros(queries.shape, jnp.float32), queries.astype(jnp.float32) * scale], axis=0
    )
    krun = jnp.concatenate([old_keys, keys], axis=0).astype(jnp.float32)
    vrun = jnp.concatenate([old_values, values], axis=0).astype(jnp.float32)
    hidden, mem_new, norm_new, m_new = cell(
        jnp.swapaxes(qrun, 0, 1),
        jnp.swapaxes(krun, 0, 1),
        jnp.swapaxes(vrun, 0, 1),
        gates.T,
        forget.T,
        memory,
        normal,
        stab,
    )
    hidden = hidden[:, props:, :]
    mean = jnp.mean(hidden, -1, keepdims=True)
    var = jnp.mean(jnp.square(hidden - mean), -1, keepdims=True)
    normed = (hidden - mean) * lax.rsqrt(var + 1e-05) * norm_gain[:, None, :]
    flat = jnp.swapaxes(normed, 0, 1).reshape(props, -1).astype(jnp.bfloat16)
    return (flat, mem_new, norm_new, m_new)


def plain_on_device(
    queries,
    keys,
    values,
    in_gate,
    forget_pre,
    old_keys,
    old_values,
    old_in_gate,
    old_forget,
    accepted,
    state_mem,
    state_norm,
    state_max,
    norm_gain,
    out_weight,
):
    mapped = jax.vmap(one_sequence, in_axes=(0, 0, 0, 0, 0, 0, 0, 0, 0, 0, 0, 0, 0, None))
    hidden, new_mem, new_norm, new_max = mapped(
        queries,
        keys,
        values,
        in_gate,
        forget_pre,
        old_keys,
        old_values,
        old_in_gate,
        old_forget,
        accepted,
        state_mem,
        state_norm,
        state_max,
        norm_gain,
    )
    terms = jnp.einsum(
        "spr,rc->spc",
        hidden,
        lax.all_gather(out_weight, "kv", axis=1, tiled=True),
        preferred_element_type=jnp.float32,
    )
    mixed = lax.psum_scatter(terms, "tp", scatter_dimension=1, tiled=True).astype(jnp.bfloat16)
    return (mixed, new_mem, new_norm, new_max)


def solution(mesh):
    kvs, tps = mesh.shape["kv"], mesh.shape["tp"]

    def step(*args):
        props, cols = args[0].shape[1], args[14].shape[1]
        fits = cols % 128 == 0 and args[0].shape[3] == 128 and kvs % PAIR == 0 and props == tps
        run = functools.partial(on_device, kvs, tps) if fits else plain_on_device
        return run(*args)

    return jax.shard_map(
        step,
        mesh=mesh,
        in_specs=(
            P("kv", None, "tp", None),
            P("kv", None, "tp", None),
            P("kv", None, "tp", None),
            P("kv", None, "tp"),
            P("kv", None, "tp"),
            P("kv", None, "tp", None),
            P("kv", None, "tp", None),
            P("kv", None, "tp"),
            P("kv", None, "tp"),
            P("kv"),
            P("kv", "tp", None, None),
            P("kv", "tp", None),
            P("kv", "tp"),
            P("tp", None),
            P("tp", "kv"),
        ),
        out_specs=(
            P("kv", "tp", None),
            P("kv", "tp", None, None),
            P("kv", "tp", None),
            P("kv", "tp"),
        ),
        check_vma=False,
    )
```

```python
import functools

import jax
import jax.numpy as jnp
from jax import lax
from jax.experimental import pallas as pl
from jax.experimental.pallas import tpu as pltpu
from jax.sharding import PartitionSpec as P

MESH = pl.DeviceIdType.MESH
F32 = jnp.float32
BF16 = jnp.bfloat16
PAIR = 2


def log_sigmoid(x):
    return jnp.minimum(x, 0.0) - jnp.log1p(jnp.exp(-jnp.abs(x)))


def split(x):
    hi = x.astype(BF16)
    return hi, (x - hi.astype(F32)).astype(BF16)


def dot(a, b):
    return jnp.dot(a, b, preferred_element_type=F32)


def kernel(
    zs, tps,
    q_ref, k_ref, v_ref, ig_ref, fg_ref, ok_ref, ov_ref, oig_ref, ofg_ref, acc_ref,
    norm_ref, max_ref, gain_ref, mem_hbm, w_hbm,
    mixed_ref, newmem_ref, newnorm_ref, newmax_ref,
    mem, w_own, w_peer, kf, vf, qf, rows, y, ck, hid, part, got,
    mem_sem, w_sem, wx_sems, hid_send, hid_recv, part_send, part_recv,
):
    seqs, heads, dk, dv = newmem_ref.shape
    props = ig_ref.shape[0]
    run = 2 * props
    stride = props * heads
    wide = dv // 128
    kv, tp = lax.axis_index("kv"), lax.axis_index("tp")
    z, x = kv // PAIR, kv % PAIR

    def device(z_at, t_at):
        return {"kv": z_at * PAIR + x, "tp": t_at}

    others = [(dz, dt) for dz in range(zs) for dt in range(tps) if dz or dt]

    def at(dz, dt):
        return lax.rem(z + dz, zs), lax.rem(tp + dt, tps)

    mem_in = [
        pltpu.make_async_copy(mem_hbm.at[s], mem.at[s], mem_sem.at[s]) for s in range(seqs)
    ]
    for copy in mem_in:
        copy.start()
    w_in = pltpu.make_async_copy(w_hbm, w_own, w_sem)
    w_in.start()

    peer = {"kv": z * PAIR + (1 - x), "tp": tp}
    barrier = pltpu.get_barrier_semaphore()
    pl.semaphore_signal(barrier, inc=1, device_id=peer, device_id_type=MESH)
    for dz, dt in others:
        pl.semaphore_signal(barrier, inc=1, device_id=device(*at(dz, dt)), device_id_type=MESH)

    accepted = acc_ref[...]
    state_max = max_ref[...]
    ig, b, total = [], [], None
    for t in range(run):
        if t < props:
            live = t < accepted
            ig.append(jnp.where(live, oig_ref[t], -jnp.inf))
            lf = jnp.where(live, log_sigmoid(ofg_ref[t]), 0.0)
        else:
            ig.append(ig_ref[t - props])
            lf = log_sigmoid(fg_ref[t - props])
        total = lf if total is None else total + lf
        b.append(total)
    index = {}
    count = 0
    for t in range(props, run):
        logd = [b[t] - b[s] + ig[s] for s in range(t + 1)]
        inter = b[t] + state_max
        m_row = functools.reduce(jnp.maximum, logd, inter)
        for s in list(range(t + 1)) + ["w"]:
            row = jnp.exp((inter if s == "w" else logd[s]) - m_row)
            rows[count * heads : (count + 1) * heads, 0:seqs] = row
            index[t, s] = count * heads
            count += 1
    newmax_ref[...] = m_row
    columns = rows[...].T[0:seqs]

    def column(t, s, h):
        return columns[:, index[t, s] + h : index[t, s] + h + 1]

    qf[...] = q_ref[...].astype(F32)
    kf[0] = ok_ref[...].astype(F32)
    kf[1] = k_ref[...].astype(F32)
    for s in range(seqs):
        for p in range(props):
            r = s * stride + p * heads
            for c in range(wide):
                lanes = slice(c * 128, (c + 1) * 128)
                vf[0, c, r : r + heads, :] = ov_ref[s, p, :, lanes].astype(F32)
                vf[1, c, r : r + heads, :] = v_ref[s, p, :, lanes].astype(F32)

    def pick(ref, p, h):
        return ref[pl.ds(p * heads + h, seqs, stride=stride), :]

    def pick_wide(ref, p, h):
        return jnp.concatenate([pick(ref.at[c], p, h) for c in range(wide)], axis=-1)

    def run_pick(ref, t, h):
        return pick(ref.at[t // props], t % props, h)

    scale = dk ** (-0.5)
    scores, dens, norms = {}, {}, {}
    for h in range(heads):
        ks = [run_pick(kf, s, h) for s in range(run)]
        normal = norm_ref[pl.ds(h, seqs, stride=heads), :]
        for t in range(props, run):
            q = pick(qf, t - props, h) * scale
            den = column(t, "w", h) * jnp.sum(q * normal, axis=-1, keepdims=True)
            for s in range(t + 1):
                score = jnp.sum(q * ks[s], axis=-1, keepdims=True) * column(t, s, h)
                scores[t, s, h] = score
                den = den + score
            dens[t, h] = jnp.maximum(jnp.abs(den), 1.0)
        norm = column(run - 1, "w", h) * normal
        for s in range(run):
            c = column(run - 1, s, h) * ks[s]
            ck.at[s // props][pl.ds((s % props) * heads + h, seqs, stride=stride), :] = c
            norm = norm + c
        newnorm_ref[pl.ds(h, seqs, stride=heads), :] = norm

    pl.semaphore_wait(barrier, len(others) + 1)
    w_swap = pltpu.make_async_remote_copy(
        src_ref=w_hbm, dst_ref=w_peer, send_sem=wx_sems.at[0], recv_sem=wx_sems.at[1],
        device_id=peer, device_id_type=MESH,
    )
    w_swap.start()

    parity = lax.broadcasted_iota(jnp.int32, (stride, 1), 0) % heads
    for s in range(seqs):
        mem_in[s].wait()
        q = q_ref[s * stride : (s + 1) * stride, :]
        out = None
        for h in range(heads):
            hi, lo = split(mem[s, h])
            term = dot(q, hi) + dot(q, lo)
            out = term if h == 0 else jnp.where(parity == h, term, out)
        for c in range(wide):
            y[c, s * stride : (s + 1) * stride, :] = out[:, c * 128 : (c + 1) * 128]

    for h in range(heads):
        vs = [pick_wide(vf.at[s // props], s % props, h) for s in range(run)]
        gain = gain_ref[h : h + 1, :]
        normed = []
        for t in range(props, run):
            num = (column(t, "w", h) * scale) * pick_wide(y, t - props, h)
            for s in range(t + 1):
                num = num + scores[t, s, h] * vs[s]
            cell = num / dens[t, h]
            mean = jnp.mean(cell, axis=-1, keepdims=True)
            cell = cell - mean
            var = jnp.mean(jnp.square(cell), axis=-1, keepdims=True)
            normed.append(cell * lax.rsqrt(var + 1e-05) * gain)
        hid[z, :, h * dv : (h + 1) * dv] = jnp.concatenate(normed, axis=0).astype(BF16)

    def hid_copy(slot, to):
        return pltpu.make_async_remote_copy(
            src_ref=hid.at[slot], dst_ref=hid.at[slot], send_sem=hid_send.at[to],
            recv_sem=hid_recv.at[slot], device_id=device(to, tp), device_id_type=MESH,
        )

    order = sorted(range(1, zs), key=lambda d: -min(d, zs - d))
    for d in order:
        hid_copy(z, lax.rem(z + d, zs)).start()

    def part_copy(slot, half, t_at, src_half):
        return pltpu.make_async_remote_copy(
            src_ref=part.at[slot, half, t_at], dst_ref=got.at[tp, z, half],
            send_sem=part_send.at[slot, half, t_at], recv_sem=part_recv.at[tp, z, half],
            device_id=device(slot, t_at), device_id_type=MESH,
        )

    def project(slot, half, weights, own):
        terms = dot(hid[slot], weights[...])
        for p in range(props):
            part[slot, half, p] = terms[p * seqs : (p + 1) * seqs].astype(BF16)
        for dt in range(tps):
            if not (own and dt == 0):
                part_copy(slot, half, lax.rem(tp + dt, tps), half).start()
        if own:
            got[tp, z, half] = part[slot, half, tp]

    w_in.wait()
    project(z, x, w_own, True)

    for s in range(seqs):
        at_s = pl.ds(s * stride, stride)
        values = jnp.concatenate(
            [
                jnp.concatenate([vf[old, c, at_s, :] for c in range(wide)], axis=-1)
                for old in (0, 1, 0, 1)
            ],
            axis=0,
        ).astype(BF16)
        keys = jnp.concatenate([ck[0, at_s, :], ck[1, at_s, :]], axis=0)
        both = lax.broadcasted_iota(jnp.int32, (2 * stride, 1), 0) % heads
        for h in range(heads):
            hi, lo = split(jnp.where(both == h, keys, 0.0))
            update = lax.dot_general(
                jnp.concatenate([hi, lo], axis=0), values, (((0,), (0,)), ((), ())),
                preferred_element_type=F32,
            )
            newmem_ref[s, h] = column(run - 1, "w", h)[s : s + 1] * mem[s, h] + update

    for d in range(1, zs):
        slot = lax.rem(z + d, zs)
        hid_copy(slot, slot).wait_recv()
        project(slot, x, w_own, False)
    w_swap.wait_recv()
    for d in range(zs):
        project(lax.rem(z + d, zs), 1 - x, w_peer, d == 0)

    for dz, dt in others:
        z_at, t_at = at(dz, dt)
        for half in range(PAIR):
            pltpu.make_async_remote_copy(
                src_ref=part.at[z_at, half, t_at], dst_ref=got.at[t_at, z_at, half],
                send_sem=part_send.at[z_at, half, t_at], recv_sem=part_recv.at[t_at, z_at, half],
                device_id=device(z_at, t_at), device_id_type=MESH,
            ).wait_recv()
    width = got.shape[-1]
    for z_at in range(zs):
        for half in range(PAIR):
            out = got[0, z_at, half].astype(F32)
            for t in range(1, tps):
                out = out + got[t, z_at, half].astype(F32)
            at_c = (z_at * PAIR + half) * width
            mixed_ref[:, at_c : at_c + width] = out.astype(BF16)

    w_swap.wait_send()
    for d in range(1, zs):
        hid_copy(z, lax.rem(z + d, zs)).wait_send()
    for dz, dt in others:
        z_at, t_at = at(dz, dt)
        for half in range(PAIR):
            part_copy(z_at, half, t_at, half).wait_send()


def on_device(
    kvs, tps,
    queries, keys, values, in_gate, forget_pre, old_keys, old_values, old_in_gate, old_forget,
    accepted, state_mem, state_norm, state_max, norm_gain, out_weight,
):
    seqs, props, heads, dk = queries.shape
    dv = values.shape[-1]
    rows, cols = out_weight.shape
    zs = kvs // PAIR
    flat = (seqs * props * heads, dk)
    gates = [jnp.transpose(g, (1, 2, 0)) for g in (in_gate, forget_pre, old_in_gate, old_forget)]
    vmem = pl.BlockSpec(memory_space=pltpu.VMEM)
    hbm = pl.BlockSpec(memory_space=pl.ANY)
    sem = pltpu.SemaphoreType.DMA
    mixed, new_mem, new_norm, new_max = pl.pallas_call(
        functools.partial(kernel, zs, tps),
        out_shape=(
            pltpu.VMEM((seqs, kvs * cols), BF16),
            pltpu.VMEM(state_mem.shape, F32),
            pltpu.VMEM((seqs * heads, dk), F32),
            pltpu.VMEM((heads, seqs), F32),
        ),
        in_specs=[vmem] * 13 + [hbm] * 2,
        out_specs=(vmem,) * 4,
        scratch_shapes=[
            pltpu.VMEM(state_mem.shape, F32),
            pltpu.VMEM((rows, cols), BF16),
            pltpu.VMEM((rows, cols), BF16),
            pltpu.VMEM((2,) + flat, F32),
            pltpu.VMEM((2, dv // 128, flat[0], 128), F32),
            pltpu.VMEM(flat, F32),
            pltpu.VMEM((128, 128), F32),
            pltpu.VMEM((dv // 128, flat[0], 128), F32),
            pltpu.VMEM((2,) + flat, F32),
            pltpu.VMEM((zs, props * seqs, heads * dv), BF16),
            pltpu.VMEM((zs, PAIR, props, seqs, cols), BF16),
            pltpu.VMEM((tps, zs, PAIR, seqs, cols), BF16),
            sem((seqs,)),
            sem,
            sem((2,)),
            sem((zs,)),
            sem((zs,)),
            sem((zs, PAIR, props)),
            sem((tps, zs, PAIR)),
        ],
        compiler_params=pltpu.CompilerParams(collective_id=0, has_side_effects=True),
    )(
        queries.reshape(flat), keys.reshape(flat), values, gates[0], gates[1],
        old_keys.reshape(flat), old_values, gates[2], gates[3], accepted.reshape(1, seqs),
        state_norm.reshape(seqs * heads, dk), state_max.T, norm_gain, state_mem, out_weight,
    )
    return (
        mixed.reshape(seqs, 1, kvs * cols),
        new_mem,
        new_norm.reshape(state_norm.shape),
        new_max.T,
    )


HIGH = lax.Precision.HIGHEST


def cell(queries, keys, values, in_gates, log_forget, memory, normal, stab):
    length = in_gates.shape[-1]
    causal = jnp.tril(jnp.ones((length, length), dtype=bool))
    cumul = jnp.cumsum(log_forget, axis=-1)
    logd = jnp.where(causal, cumul[:, :, None] - cumul[:, None, :] + in_gates[:, None, :], -jnp.inf)
    inter = cumul + stab[:, None]
    m_row = jnp.maximum(inter, jnp.max(logd, axis=-1))
    scores = jnp.einsum("hld,hsd->hls", queries, keys, precision=HIGH) * jnp.exp(
        logd - m_row[..., None]
    )
    w_inter = jnp.exp(inter - m_row)
    num = w_inter[..., None] * jnp.einsum(
        "hld,hde->hle", queries, memory, precision=HIGH
    ) + jnp.einsum("hls,hse->hle", scores, values, precision=HIGH)
    den = w_inter * jnp.einsum("hld,hd->hl", queries, normal, precision=HIGH) + jnp.sum(
        scores, axis=-1
    )
    hidden = num / jnp.maximum(jnp.abs(den), 1.0)[..., None]
    m_new = m_row[:, -1]
    g_state = jnp.exp(cumul[:, -1] + stab - m_new)
    g_tok = jnp.exp(cumul[:, -1:] - cumul + in_gates - m_new[:, None])
    mem_new = g_state[:, None, None] * memory + jnp.einsum(
        "hld,hle->hde", g_tok[..., None] * keys, values, precision=HIGH
    )
    norm_new = g_state[:, None] * normal + jnp.einsum("hl,hld->hd", g_tok, keys, precision=HIGH)
    return (hidden, mem_new, norm_new, m_new)


def one_sequence(
    queries,
    keys,
    values,
    in_gate,
    forget_pre,
    old_keys,
    old_values,
    old_in_gate,
    old_forget,
    accepted,
    memory,
    normal,
    stab,
    norm_gain,
):
    props = queries.shape[0]
    live = jnp.arange(props, dtype=jnp.int32) < accepted
    gates = jnp.concatenate([jnp.where(live[:, None], old_in_gate, -jnp.inf), in_gate], axis=0)
    forget = jnp.concatenate(
        [
            jnp.where(live[:, None], jax.nn.log_sigmoid(old_forget), 0.0),
            jax.nn.log_sigmoid(forget_pre),
        ],
        axis=0,
    )
    scale = queries.shape[-1] ** (-0.5)
    qrun = jnp.concatenate(
        [jnp.zeros(queries.shape, jnp.float32), queries.astype(jnp.float32) * scale], axis=0
    )
    krun = jnp.concatenate([old_keys, keys], axis=0).astype(jnp.float32)
    vrun = jnp.concatenate([old_values, values], axis=0).astype(jnp.float32)
    hidden, mem_new, norm_new, m_new = cell(
        jnp.swapaxes(qrun, 0, 1),
        jnp.swapaxes(krun, 0, 1),
        jnp.swapaxes(vrun, 0, 1),
        gates.T,
        forget.T,
        memory,
        normal,
        stab,
    )
    hidden = hidden[:, props:, :]
    mean = jnp.mean(hidden, -1, keepdims=True)
    var = jnp.mean(jnp.square(hidden - mean), -1, keepdims=True)
    normed = (hidden - mean) * lax.rsqrt(var + 1e-05) * norm_gain[:, None, :]
    flat = jnp.swapaxes(normed, 0, 1).reshape(props, -1).astype(jnp.bfloat16)
    return (flat, mem_new, norm_new, m_new)


def plain_on_device(
    queries,
    keys,
    values,
    in_gate,
    forget_pre,
    old_keys,
    old_values,
    old_in_gate,
    old_forget,
    accepted,
    state_mem,
    state_norm,
    state_max,
    norm_gain,
    out_weight,
):
    mapped = jax.vmap(one_sequence, in_axes=(0, 0, 0, 0, 0, 0, 0, 0, 0, 0, 0, 0, 0, None))
    hidden, new_mem, new_norm, new_max = mapped(
        queries,
        keys,
        values,
        in_gate,
        forget_pre,
        old_keys,
        old_values,
        old_in_gate,
        old_forget,
        accepted,
        state_mem,
        state_norm,
        state_max,
        norm_gain,
    )
    terms = jnp.einsum(
        "spr,rc->spc",
        hidden,
        lax.all_gather(out_weight, "kv", axis=1, tiled=True),
        preferred_element_type=jnp.float32,
    )
    mixed = lax.psum_scatter(terms, "tp", scatter_dimension=1, tiled=True).astype(jnp.bfloat16)
    return (mixed, new_mem, new_norm, new_max)


def solution(mesh):
    kvs, tps = mesh.shape["kv"], mesh.shape["tp"]

    def step(*args):
        props, cols = args[0].shape[1], args[14].shape[1]
        fits = cols % 128 == 0 and args[0].shape[3] == 128 and kvs % PAIR == 0 and props == tps
        run = functools.partial(on_device, kvs, tps) if fits else plain_on_device
        return run(*args)

    return jax.shard_map(
        step,
        mesh=mesh,
        in_specs=(
            P("kv", None, "tp", None),
            P("kv", None, "tp", None),
            P("kv", None, "tp", None),
            P("kv", None, "tp"),
            P("kv", None, "tp"),
            P("kv", None, "tp", None),
            P("kv", None, "tp", None),
            P("kv", None, "tp"),
            P("kv", None, "tp"),
            P("kv"),
            P("kv", "tp", None, None),
            P("kv", "tp", None),
            P("kv", "tp"),
            P("tp", None),
            P("tp", "kv"),
        ),
        out_specs=(
            P("kv", "tp", None),
            P("kv", "tp", None, None),
            P("kv", "tp", None),
            P("kv", "tp"),
        ),
        check_vma=False,
    )
```
